32 devices in a mesh: ep: 4 (over y, x), tp: 8 (over z, core).
Axes of the slice: x: 2, y: 2, z: 4, core: 2. Of those that a mesh axis runs over, the one named last changes fastest.
Arguments:
- queries: bfloat16 [4096, 2048], P('ep', 'tp'), may hold values from -200 to 200
- key_rows: bfloat16 [4096, 1024], P('ep', 'tp'), may hold values from -6 to 6
- value_rows: bfloat16 [4096, 1024], P('ep', 'tp'), may hold values from -24 to 24
- sink_logits: float32 [32], P('tp'), may hold values from 2 to 6
- out_weight: bfloat16 [2048, 2048], P('tp'), may hold values from -0.125 to 0.125
- expert_input: bfloat16 [3072, 2048], P(('ep', 'tp')), may hold values from -6 to 6
- norm_gain: float32 [2048], replicated, may hold values from 0.1 to 1.9
- group_ids: int32 [3072, 1], P(('ep', 'tp')), may hold values from 0 to 3; in each aligned block of 96 rows (0 to 95, 96 to 191, ...) at most 30 rows name the same one
- route_weight: float32 [3072, 2], P(('ep', 'tp')), may hold values from 0.2 to 1
- gate_weight: bfloat16 [8, 2048, 4096], P('ep', None, 'tp'), may hold values from -0.125 to 0.125
- up_weight: bfloat16 [8, 2048, 4096], P('ep', None, 'tp'), may hold values from -0.125 to 0.125
- down_weight: bfloat16 [8, 4096, 2048], P('ep', 'tp'), may hold values from -0.09375 to 0.09375
Outputs:
- attn_output: bfloat16 [4096, 2048], P(('ep', 'tp'))
- expert_output: bfloat16 [3072, 2048], P(('ep', 'tp'))
The draws below stay inside these ranges and needn't reach their ends.
Inputs may be any that keep to these rules, and one draw needn't show every extreme that they name: `group_ids`: in the rows of one device (aligned blocks of 96 rows), no group is named by more than 30 rows, and in every draw some group is named by exactly 30 rows of some block.
All inputs are finite; a program needn't handle non-finite values.
Results may differ from the reference program's by a relative error of at most 0.02.
Values may be sent and summed in bfloat16 or wider, within the bound.
A program may use at most 128 MiB of HBM per device.

```python
import math
import jax
import jax.numpy as jnp
import numpy as np
from jax import lax

D = 2048
HD = 64
HEADS = 32
KV_HEADS = 16
WINDOW = 128
DE = 4096
EXP_DEV = 2
TB = 96
EXPERTS = 8
CAP = 30
TOK_A = 4096
TOK_B = 3072
N_EP = 4
N_TP = 8


def drawn_keys(key):
    base_keys = jax.random.normal(jax.random.fold_in(key, 11), (TOK_A, KV_HEADS, HD), jnp.float32)
    return jnp.clip(base_keys, -6.0, 6.0)


def draw_key_rows(key, part):
    return drawn_keys(key).reshape(TOK_A, KV_HEADS * HD).astype(jnp.bfloat16)


def draw_queries(key, part):
    fresh = jax.random.normal(jax.random.fold_in(key, 21), (TOK_A, HEADS, HD), jnp.float32)
    fresh = jnp.clip(fresh, -6.0, 6.0)
    return fresh.reshape(TOK_A, HEADS * HD).astype(jnp.bfloat16)


def block_scale(stream_key, dims, shards, smallest, top_value):
    def one(dim, blocks):
        draws = jax.random.uniform(jax.random.fold_in(jax.random.fold_in(stream_key, 6), dim), (blocks,), jnp.float32, smallest / len(shards), top_value / len(shards))
        return jnp.repeat(jnp.exp(draws), dims[dim] // blocks).reshape((-1,) + (1,) * (len(dims) - dim - 1))

    gain = one(*shards[0])
    for cut in shards[1:]:
        gain = gain * one(*cut)
    return gain


def routed_block(own_key, own, number, rows, count, top, reach, slope):
    sequence = jax.random.permutation(own_key, count)
    crowded, common = load_shares(count, rows * top, reach, slope, True), load_shares(count, rows * top, reach, slope, False)
    places = jnp.arange(count)

    def named(lengths, rotation):
        used = int((lengths > 0).sum())
        fixed = max(1, used // 4)
        passed = fixed + (places - fixed + rotation * (used - fixed)) % max(1, count - fixed)
        return jnp.zeros((count,), jnp.int32).at[sequence[jnp.where(places < fixed, places, passed)]].set(jnp.asarray(lengths, jnp.int32))

    lengths = jnp.where(number % 4 == 0, named(crowded, number // 4), named(common, number - number // 4 - 1))
    mixed = jax.random.permutation(jax.random.fold_in(own, 3), count)
    donor, sink = mixed[0:count // 2 * 2:2], mixed[1:count // 2 * 2:2]
    slack = jnp.minimum(lengths[donor] - 1, reach - lengths[sink]) // 2
    slack = jnp.where((donor == sequence[0]) | (sink == sequence[0]) | (lengths[sink] == 0), 0, jnp.maximum(slack, 0))
    passed = jax.random.randint(jax.random.fold_in(own, 4), (count // 2,), 0, 1 << 20) % (slack + 1)
    lengths = lengths.at[donor].add(-passed).at[sink].add(passed)
    labels = jnp.searchsorted(jnp.cumsum(lengths), jnp.arange(rows * top), side="right").astype(jnp.int32)
    table = labels.reshape(top, rows).T
    table = table[jax.random.permutation(jax.random.fold_in(own, 1), rows)]
    rotation = jax.random.randint(jax.random.fold_in(own, 2), (rows, 1), 0, top)
    return jnp.take_along_axis(table, (jnp.arange(top)[None, :] + rotation) % top, axis=1)


def load_shares(number_of, total, reach, skew, full):
    loads = [(1 << 20) // math.isqrt(standing ** skew) + 1 for standing in range(1, number_of + 1)]
    largest = reach if full else min(reach, max(-(-total // number_of), total * loads[0] // sum(loads)))
    least = 1 if total - largest >= number_of - 1 else 0
    holding, spare = [largest] + [least] * (number_of - 1), total - largest - least * (number_of - 1)
    while spare > 0:
        free = [i for i in range(1, number_of) if holding[i] < largest] or [i for i in range(1, number_of) if holding[i] < reach]
        whole, remaining = sum([loads[i] for i in free]), spare
        for i in free:
            extra = min(reach - holding[i], max(1, remaining * loads[i] // whole), spare)
            holding[i] = holding[i] + extra
            spare = spare - extra
    return np.array(holding)


def bell_draw(key, shape, spread, most, pieces=(), kind=jnp.bfloat16):
    result = jax.random.normal(key, shape, jnp.float32) * spread
    if len(pieces) > 0:
        result = block_scale(key, shape, pieces, -0.22, 0.18) * result
    return jnp.clip(result, min=-most, max=most).astype(kind)


def setup_inputs(seed: int = 0) -> dict:
    key_of = jax.random.split(jax.random.key(seed), 13)
    queries = draw_queries(jax.random.fold_in(key_of[12], 71), 0)
    key_rows = draw_key_rows(jax.random.fold_in(key_of[12], 71), 0)
    value_rows = bell_draw(key_of[2], (TOK_A, KV_HEADS * HD), 4.0, 24.0, ((0, 4), (1, 8)))
    sink_logits = jnp.clip(2.0 + 4.0 * jax.random.uniform(key_of[3], (HEADS,), jnp.float32) ** block_scale(key_of[3], (HEADS,), ((0, 8),), -0.2, 0.2), 2.0, 6.0)
    out_weight = bell_draw(key_of[4], (HEADS * HD, D), (HEADS * HD) ** -0.5, 0.125, ((0, 8),))
    expert_input = bell_draw(key_of[5], (TOK_B, D), 1.0, 6.0, ((0, 32),))
    norm_gain = jnp.clip(1.0 + 0.18 * jax.random.normal(key_of[6], (D,), jnp.float32), 0.1, 1.9)
    group_ids_keys = jax.random.split(jax.random.fold_in(key_of[7], 1), TOK_B // TB)
    group_ids_turns = jax.random.permutation(jax.random.fold_in(key_of[7], 3), TOK_B // TB)
    group_ids = jax.vmap(lambda own, number: routed_block(jax.random.fold_in(key_of[7], 2), own, number, TB, N_EP, 1, CAP, 2))(group_ids_keys, group_ids_turns).reshape((TOK_B, 1))
    route_weight = jnp.clip(0.2 + 0.8 * jax.random.uniform(key_of[8], (TOK_B, EXP_DEV), jnp.float32) ** block_scale(key_of[8], (TOK_B, EXP_DEV), ((0, 32),), -0.2, 0.2), 0.2, 1.0)
    gate_weight = bell_draw(key_of[9], (EXPERTS, D, DE), D ** -0.5, 0.125, ((0, 4), (2, 8)))
    up_weight = bell_draw(key_of[10], (EXPERTS, D, DE), D ** -0.5, 0.125, ((0, 4), (2, 8)))
    down_weight = bell_draw(key_of[11], (EXPERTS, DE, D), DE ** -0.5, 0.09375, ((0, 4), (1, 8)))
    return {"queries": queries, "key_rows": key_rows, "value_rows": value_rows, "sink_logits": sink_logits, "out_weight": out_weight, "expert_input": expert_input, "norm_gain": norm_gain, "group_ids": group_ids, "route_weight": route_weight, "gate_weight": gate_weight, "up_weight": up_weight, "down_weight": down_weight}


theta_base = 10000.0
norm_eps = 1e-06
neg_large = -1e+30

def rotate(tensor, positions):
    halfway = tensor.shape[-1] // 2
    frequency = theta_base ** (-(jnp.arange(halfway, dtype=jnp.float32) * 2.0) / tensor.shape[-1])
    angles = positions.astype(jnp.float32)[:, None] * frequency[None, :]
    cosine = jnp.cos(angles)[:, None, :]
    sine_part = jnp.sin(angles)[:, None, :]
    front_part = tensor[..., :halfway]
    back_part = tensor[..., halfway:]
    return jnp.concatenate([front_part * cosine - back_part * sine_part, back_part * cosine + front_part * sine_part], axis=-1)

def attention(queries, key_rows, value_rows, sink_logits, out_weight):
    tokens = queries.shape[0]
    per_group = HEADS // KV_HEADS
    positions = jnp.arange(tokens, dtype=jnp.int32)
    rot_query = rotate(queries.astype(jnp.float32).reshape(tokens, HEADS, HD), positions).astype(jnp.bfloat16)
    rot_key = rotate(key_rows.astype(jnp.float32).reshape(tokens, KV_HEADS, HD), positions).astype(jnp.bfloat16)
    value_heads = value_rows.reshape(tokens, KV_HEADS, HD)
    key_padded = jnp.concatenate([jnp.zeros((WINDOW, KV_HEADS, HD), jnp.bfloat16), rot_key], axis=0)
    value_padded = jnp.concatenate([jnp.zeros((WINDOW, KV_HEADS, HD), jnp.bfloat16), value_heads], axis=0)
    score_scale = 1.0 / math.sqrt(HD)
    row_ids = jnp.arange(WINDOW, dtype=jnp.int32)[:, None]
    col_ids = jnp.arange(2 * WINDOW, dtype=jnp.int32)[None, :]
    lagged = row_ids + WINDOW - col_ids
    sink_col = sink_logits.astype(jnp.float32).reshape(KV_HEADS, per_group, 1, 1)

    def one_block(block_id):
        begin = (block_id * WINDOW).astype(jnp.int32)
        query_blk = lax.dynamic_slice_in_dim(rot_query, begin, WINDOW, 0).reshape(WINDOW, KV_HEADS, per_group, HD)
        key_blk = lax.dynamic_slice_in_dim(key_padded, begin, 2 * WINDOW, 0)
        value_blk = lax.dynamic_slice_in_dim(value_padded, begin, 2 * WINDOW, 0)
        scores = jnp.einsum('qkgd,skd->kgqs', query_blk.astype(jnp.float32), key_blk.astype(jnp.float32)) * score_scale
        key_pos = begin - WINDOW + col_ids
        allowed = (lagged >= 0) & (lagged < WINDOW) & (key_pos >= 0)
        scores = jnp.where(allowed[None, None], scores, neg_large)
        top_val = jnp.maximum(lax.optimization_barrier(jnp.max(scores, axis=-1, keepdims=True)), sink_col)
        expo = jnp.exp(scores - top_val)
        denom = lax.optimization_barrier(jnp.sum(expo, axis=-1, keepdims=True)) + jnp.exp(sink_col - top_val)
        probs = (expo / denom).astype(jnp.bfloat16)
        mixed = jnp.einsum('kgqs,skd->qkgd', probs.astype(jnp.float32), value_blk.astype(jnp.float32))
        return mixed.reshape(WINDOW, HEADS * HD).astype(jnp.bfloat16)
    attended = lax.map(one_block, jnp.arange(tokens // WINDOW, dtype=jnp.int32)).reshape(tokens, HEADS * HD)
    group_cols = HEADS * HD // N_TP

    def add_group(total, group_id):
        cols = lax.dynamic_slice_in_dim(attended, group_id * group_cols, group_cols, 1)
        rows_w = lax.dynamic_slice_in_dim(out_weight, group_id * group_cols, group_cols, 0)
        partial_sum = jnp.dot(cols, rows_w, preferred_element_type=jnp.float32).astype(jnp.bfloat16)
        partial_sum = lax.optimization_barrier(partial_sum)
        return (total + partial_sum.astype(jnp.float32), None)
    total, unused = lax.scan(add_group, jnp.zeros((tokens, D), jnp.float32), jnp.arange(N_TP, dtype=jnp.int32))
    return total.astype(jnp.bfloat16)

def experts(expert_input, norm_gain, group_ids, route_weight, gate_weight, up_weight, down_weight):
    tokens = expert_input.shape[0]
    as_float = expert_input.astype(jnp.float32)
    normed = (as_float * lax.rsqrt(lax.optimization_barrier(jnp.mean(as_float * as_float, axis=-1, keepdims=True)) + norm_eps) * norm_gain).astype(jnp.bfloat16)
    shares = lax.optimization_barrier(route_weight.astype(jnp.bfloat16)).astype(jnp.float32)
    chosen = group_ids[:, 0].astype(jnp.int32)
    nblocks = tokens // TB
    onehot = (chosen.reshape(nblocks, TB)[:, :, None] == jnp.arange(N_EP, dtype=jnp.int32)[None, None, :]).astype(jnp.int32)
    ranks = lax.optimization_barrier(jnp.sum((jnp.cumsum(onehot, axis=1) - onehot) * onehot, axis=-1)).reshape(tokens)
    block_of = jnp.arange(tokens, dtype=jnp.int32) // TB
    dest = ((chosen * nblocks + block_of) * CAP + ranks).astype(jnp.int32)
    slots = N_EP * nblocks * CAP
    slot_rows = jnp.zeros((slots, D), jnp.bfloat16).at[dest].set(normed)
    slot_shares = jnp.zeros((slots, EXP_DEV), jnp.float32).at[dest].set(shares)
    per_group = nblocks * CAP
    unit_group = DE // N_TP

    def one_group(args):
        rows_in, shares_in, group_id = args
        first = (group_id * EXP_DEV).astype(jnp.int32)
        gate_w = lax.dynamic_slice_in_dim(gate_weight, first, EXP_DEV, 0).astype(jnp.float32)
        up_w = lax.dynamic_slice_in_dim(up_weight, first, EXP_DEV, 0).astype(jnp.float32)
        down_w = lax.dynamic_slice_in_dim(down_weight, first, EXP_DEV, 0)
        rows_f = rows_in.astype(jnp.float32)
        gate_val = jnp.einsum('rd,edf->ref', rows_f, gate_w)
        up_val = jnp.einsum('rd,edf->ref', rows_f, up_w)
        hidden = (jax.nn.silu(gate_val) * up_val * shares_in[:, :, None]).astype(jnp.bfloat16)

        def add_units(total, unit_id):
            hid_part = lax.dynamic_slice_in_dim(hidden, unit_id * unit_group, unit_group, 2).astype(jnp.float32)
            down_part = lax.dynamic_slice_in_dim(down_w, unit_id * unit_group, unit_group, 1).astype(jnp.float32)
            partial_sum = jnp.einsum('ref,efd->rd', hid_part, down_part).astype(jnp.bfloat16)
            partial_sum = lax.optimization_barrier(partial_sum)
            return (total + partial_sum.astype(jnp.float32), None)
        total, unused = lax.scan(add_units, jnp.zeros((per_group, D), jnp.float32), jnp.arange(N_TP, dtype=jnp.int32))
        return total.astype(jnp.bfloat16)
    results = lax.map(one_group, (slot_rows.reshape(N_EP, per_group, D), slot_shares.reshape(N_EP, per_group, EXP_DEV), jnp.arange(N_EP, dtype=jnp.int32)))
    return results.reshape(slots, D)[dest]

def reference(queries, key_rows, value_rows, sink_logits, out_weight, expert_input, norm_gain, group_ids, route_weight, gate_weight, up_weight, down_weight):
    attn_output = attention(queries, key_rows, value_rows, sink_logits, out_weight)
    expert_output = experts(expert_input, norm_gain, group_ids, route_weight, gate_weight, up_weight, down_weight)
    return (attn_output, expert_output)
```

```python
import math

import jax
import jax.numpy as jnp
from jax import lax
from jax.sharding import PartitionSpec as P

D = 2048
HD = 64
WINDOW = 128
EXP_DEV = 2


theta_base = 10000.0
norm_eps = 1e-06
neg_large = -1e30


def shifted(shard, axis, by):
    length = lax.axis_size(axis)
    pairs = [(i, i + by) for i in range(length) if 0 <= i + by < length]
    return lax.ppermute(shard, axis, pairs)


def rotate(tensor, positions):
    halfway = tensor.shape[-1] // 2
    frequency = theta_base ** (-(jnp.arange(halfway, dtype=jnp.float32) * 2.0) / tensor.shape[-1])
    angles = positions.astype(jnp.float32)[:, None] * frequency[None, :]
    cosine = jnp.cos(angles)[:, None, :]
    sine_part = jnp.sin(angles)[:, None, :]
    front_part = tensor[..., :halfway]
    back_part = tensor[..., halfway:]
    return jnp.concatenate(
        [front_part * cosine - back_part * sine_part, back_part * cosine + front_part * sine_part],
        axis=-1,
    )


def banded(earlier, current, nblocks):
    kv_here = current.shape[1]
    joined = jnp.concatenate([earlier, current[: current.shape[0] - WINDOW]], axis=0)
    joined = joined.reshape(nblocks, WINDOW, kv_here, HD)
    return jnp.concatenate([joined, current.reshape(nblocks, WINDOW, kv_here, HD)], axis=1)


def bands(queries, key_rows, value_rows, sink_logits):
    seg_rows = queries.shape[0]
    heads_here = sink_logits.shape[0]
    kv_here = key_rows.shape[1] // HD
    per_group = heads_here // kv_here
    nblocks = seg_rows // WINDOW
    offset = lax.axis_index("ep") * seg_rows
    positions = offset + jnp.arange(seg_rows, dtype=jnp.int32)
    rot_query = rotate(
        queries.astype(jnp.float32).reshape(seg_rows, heads_here, HD), positions
    ).astype(jnp.bfloat16)
    rot_key = rotate(key_rows.astype(jnp.float32).reshape(seg_rows, kv_here, HD), positions).astype(
        jnp.bfloat16
    )
    value_heads = value_rows.reshape(seg_rows, kv_here, HD)
    tails = jnp.stack([rot_key[seg_rows - WINDOW :], value_heads[seg_rows - WINDOW :]]).reshape(
        2, WINDOW, kv_here * HD
    )
    before = shifted(tails, "ep", 1).reshape(2, WINDOW, kv_here, HD)
    key_band = banded(before[0], rot_key, nblocks)
    value_band = banded(before[1], value_heads, nblocks)
    grouped_query = rot_query.reshape(nblocks, WINDOW, kv_here, per_group, HD)
    return grouped_query, key_band, value_band


def attend(grouped_query, key_band, value_band, sink_logits):
    nblocks, _, kv_here, per_group, _ = grouped_query.shape
    heads_here = kv_here * per_group
    seg_rows = nblocks * WINDOW
    offset = lax.axis_index("ep") * seg_rows
    score_scale = 1.0 / math.sqrt(HD)
    scores = (
        jnp.einsum("nqkgd,nskd->nkgqs", grouped_query, key_band, preferred_element_type=jnp.float32)
        * score_scale
    )
    row_ids = jnp.arange(WINDOW, dtype=jnp.int32)[:, None]
    col_ids = jnp.arange(2 * WINDOW, dtype=jnp.int32)[None, :]
    lagged = row_ids + WINDOW - col_ids
    key_pos = (
        offset
        + (jnp.arange(nblocks, dtype=jnp.int32) * WINDOW)[:, None, None]
        - WINDOW
        + col_ids[None]
    )
    allowed = (lagged >= 0)[None] & (lagged < WINDOW)[None] & (key_pos >= 0)
    scores = jnp.where(allowed[:, None, None], scores, neg_large)
    sink_col = sink_logits.reshape(1, kv_here, per_group, 1, 1)
    top_val = jnp.maximum(jnp.max(scores, axis=-1, keepdims=True), sink_col)
    expo = jnp.exp(scores - top_val)
    denom = jnp.sum(expo, axis=-1, keepdims=True) + jnp.exp(sink_col - top_val)
    probs = (expo / denom).astype(jnp.bfloat16)
    attended = jnp.einsum(
        "nkgqs,nskd->nqkgd", probs, value_band, preferred_element_type=jnp.float32
    )
    attended = attended.astype(jnp.bfloat16).reshape(seg_rows, heads_here * HD)
    return attended


def xor_send(tensor, axis, mask):
    pairs = [(i, i ^ mask) for i in range(lax.axis_size(axis))]
    return lax.ppermute(tensor, axis, pairs)


def z_send(tensor, hop, keep):
    n_z = lax.axis_size("tp") // 2
    pairs = [
        (2 * z + c, 2 * (z + hop) + c)
        for z in range(n_z)
        for c in range(2)
        if 0 <= z + hop < n_z and keep(z)
    ]
    return lax.ppermute(tensor, "tp", pairs)


def together(*values):
    return lax.optimization_barrier(values)


class Reduction:
    def __init__(self, piece):
        self.piece, self.terms = piece, {}
        self.n_z = lax.axis_size("tp") // 2
        self.got = None

    def term(self, d):
        if d not in self.terms:
            self.terms[d] = self.piece(d)
        return self.terms[d]

    def outgoing(self, s):
        pair = [self.term(self.n_z - s), self.term(s)]
        if self.got is not None:
            pair = [p + g.astype(jnp.float32) for p, g in zip(pair, self.got)]
        return tuple(p.astype(jnp.bfloat16) for p in pair)

    def send(self, s, pair):
        n_z = self.n_z
        self.got = (
            z_send(pair[0], 1, lambda i: i <= s - 1),
            z_send(pair[1], -1, lambda i: i >= n_z - s),
        )

    def result(self):
        up, down = self.got
        return (self.piece(0) + up.astype(jnp.float32) + down.astype(jnp.float32)).astype(
            jnp.bfloat16
        )


def project(attended, out_weight, weight_pair):
    n_tp = lax.axis_size("tp")
    me = lax.axis_index("tp")
    rows = attended.shape[0] // n_tp

    n_z = n_tp // 2

    def half(core):
        order = [(me // 2 + d) % n_z * 2 + core for d in range(n_z)]
        return jnp.concatenate(
            [lax.dynamic_slice_in_dim(attended, t * rows, rows, 0) for t in order], axis=0
        )

    theirs = xor_send(half(1 - me % 2), "tp", 1)
    pooled = jnp.concatenate([half(me % 2), theirs], axis=1)
    weight = jnp.concatenate([out_weight, weight_pair], axis=0)
    part = jnp.dot(pooled, weight, preferred_element_type=jnp.float32).astype(jnp.bfloat16)
    return part, rows


def route(expert_input, norm_gain, group_ids, route_weight):
    token_count = expert_input.shape[0]
    n_groups = lax.axis_size("ep")
    me = lax.axis_index("ep")
    capacity = max(2, token_count * 5 // (4 * n_groups))
    padded = -(-(capacity + EXP_DEV) // 16) * 16
    as_float = expert_input.astype(jnp.float32)
    normed = (
        as_float
        * lax.rsqrt(jnp.mean(as_float * as_float, axis=-1, keepdims=True) + norm_eps)
        * norm_gain
    ).astype(jnp.bfloat16)
    chosen = group_ids[:, 0] ^ me
    onehot = (chosen[:, None] == jnp.arange(n_groups, dtype=jnp.int32)[None, :]).astype(jnp.int32)
    order = jnp.arange(token_count, dtype=jnp.int32)
    before = (order[:, None] > order[None, :]) & (chosen[:, None] == chosen[None, :])
    ranks = jnp.sum(before.astype(jnp.int32), axis=1)
    slot_of = chosen * padded + ranks
    slots = n_groups * padded
    picker = (jnp.arange(slots, dtype=jnp.int32)[:, None] == slot_of[None, :]).astype(jnp.bfloat16)
    rows = jnp.dot(picker, normed, preferred_element_type=jnp.float32).astype(jnp.bfloat16)
    shares = lax.dot_general(
        route_weight.astype(jnp.bfloat16), picker, (((0,), (1,)), ((), ())),
        preferred_element_type=jnp.float32,
    ).astype(jnp.bfloat16)
    rows = rows.reshape(n_groups, padded, D)
    shares = shares.reshape(EXP_DEV, n_groups, padded).transpose(1, 0, 2)
    shares = jnp.pad(shares, ((0, 0), (padded - EXP_DEV, 0), (0, D - padded)))
    return rows + shares, picker


def hidden_units(rows, groups, gate_weight, up_weight):
    padded = rows.shape[0] // groups
    spare = rows.reshape(groups, padded, D)[:, padded - EXP_DEV :, :padded]
    shares = spare.transpose(0, 2, 1).reshape(rows.shape[0], EXP_DEV).astype(jnp.float32)
    hidden = []
    for e in range(EXP_DEV):
        gate_val = jnp.dot(rows, gate_weight[e], preferred_element_type=jnp.float32)
        up_val = jnp.dot(rows, up_weight[e], preferred_element_type=jnp.float32)
        hidden.append(
            (jax.nn.silu(gate_val) * up_val * shares[:, e : e + 1]).astype(jnp.bfloat16)
        )
    return jnp.concatenate(hidden, axis=1)


def return_rows(total, picker, n_groups):
    combined = total.reshape(n_groups, -1, D)
    back = [combined[0]] + [xor_send(combined[k], "ep", k) for k in range(1, n_groups)]
    gathered = jnp.einsum(
        "sr,sd->rd", picker, jnp.concatenate(back, axis=0), preferred_element_type=jnp.float32
    )
    return gathered.astype(jnp.bfloat16)


def body(
    queries,
    key_rows,
    value_rows,
    sink_logits,
    out_weight,
    expert_input,
    norm_gain,
    group_ids,
    route_weight,
    gate_weight,
    up_weight,
    down_weight,
):
    n_tp = lax.axis_size("tp")
    n_z = n_tp // 2
    z = lax.axis_index("tp") // 2
    n_groups = lax.axis_size("ep")
    weight_pair = xor_send(out_weight, "tp", 1)
    down_pair = xor_send(down_weight, "tp", 1)
    rows, picker = route(expert_input, norm_gain, group_ids, route_weight)
    band = bands(queries, key_rows, value_rows, sink_logits)
    got = [rows[0]] + [xor_send(rows[k], "ep", k) for k in range(1, n_groups)]
    own = jnp.concatenate(got, axis=0)
    local = own.shape[0]

    up, down = own, own
    ups, downs = [], []
    sums = None
    for s in range(1, n_z):
        if s == 2:
            up, down, *band = together(up, down, *band)
        if s == max(2, n_z - 1):
            attended = attend(*band, sink_logits)
            part, out_rows = project(attended, out_weight, weight_pair)
            sums = Reduction(
                lambda d: part[d * out_rows : (d + 1) * out_rows].astype(jnp.float32)
            )
            up, down, part = together(up, down, part)
            first_sums = sums.outgoing(1)
        up = z_send(up, 1, lambda i: i >= s - 1)
        down = z_send(down, -1, lambda i: i <= n_z - s)
        ups.append(up)
        downs.append(down)
    sums.send(1, first_sums)
    from_back = [None] + [jnp.where(z >= d, ups[d - 1], downs[n_z - d - 1]) for d in range(1, n_z)]
    nearest = jnp.where(z >= 1, ups[0], downs[0])
    last = jnp.where(z >= 1, from_back[n_z - 1], from_back[1])
    chunks = [own, nearest] + from_back[2 : n_z - 1] + [last]
    pairs = [xor_send(c, "tp", 1) for c in chunks]
    early = jnp.concatenate(chunks[:2] + pairs[:2], axis=0)
    late = jnp.concatenate(chunks[2:] + pairs[2:], axis=0)
    if n_z > 2:
        early, *second = together(early, *sums.outgoing(2))
        sums.send(2, second)
    hidden_early = hidden_units(early, 4 * n_groups, gate_weight, up_weight)
    if n_z > 3:
        late, hidden_early, *third = together(late, hidden_early, *sums.outgoing(3))
        sums.send(3, third)
    hidden_late = hidden_units(late, 2 * (n_z - 2) * n_groups, gate_weight, up_weight)
    cut, units = 2 * local, hidden_early.shape[1]
    rest = (n_z - 2) * local
    mine = jnp.concatenate([hidden_early[:cut], hidden_late[:rest]], axis=0)
    theirs = jnp.concatenate(
        [xor_send(hidden_early[cut:], "tp", 1), xor_send(hidden_late[rest:], "tp", 1)], axis=0
    )
    for s in range(4, n_z):
        pair = sums.outgoing(s)
        mine, *pair = together(mine, *pair)
        sums.send(s, pair)
    down_all = jnp.concatenate(
        [down_weight.reshape(units, D), down_pair.reshape(units, D)], axis=0
    )
    pooled = jnp.concatenate([mine, theirs], axis=1)

    def piece(j):
        d = (z - (z ^ j)) % n_z
        swapped = jnp.where((d == 1) | (d == n_z - 1), n_z - d, d)
        block = lax.dynamic_slice_in_dim(pooled, jnp.where(z >= 1, d, swapped) * local, local, 0)
        return jnp.dot(block, down_all, preferred_element_type=jnp.float32)

    sent = [
        xor_send(piece(j).astype(jnp.bfloat16), "tp", 2 * j)
        for j in sorted(range(1, n_z), key=lambda j: -j)
    ]
    total = lax.dynamic_slice_in_dim(pooled, 0, local, 0)
    total = jnp.dot(total, down_all, preferred_element_type=jnp.float32)
    for term in sent:
        total = total + term.astype(jnp.float32)
    total = total.astype(jnp.bfloat16)
    expert_output = return_rows(total, picker, n_groups)
    attn_output = sums.result()
    return (attn_output, expert_output)


def solution(mesh):
    placed = (
        P("ep", "tp"),
        P("ep", "tp"),
        P("ep", "tp"),
        P("tp"),
        P("tp", None),
        P(("ep", "tp"), None),
        P(),
        P(("ep", "tp"), None),
        P(("ep", "tp"), None),
        P("ep", None, "tp"),
        P("ep", None, "tp"),
        P("ep", "tp", None),
    )
    return jax.shard_map(
        body,
        mesh=mesh,
        in_specs=placed,
        out_specs=(P(("ep", "tp"), None), P(("ep", "tp"), None)),
        check_vma=False,
    )
```
